32 devices in a mesh: ep: 8 (over z, x), tp: 4 (over y, core).
Axes of the slice: x: 2, y: 2, z: 4, core: 2. Of those that a mesh axis runs over, the one named last changes fastest.
Arguments:
- mixer_input: bfloat16 [4096, 2048], P('ep', 'tp'), may hold values from -6 to 6
- mixer_gain: float32 [2048], replicated, may hold values from 0.1 to 1.9
- w_query: bfloat16 [2048, 1024], P(None, 'tp'), may hold values from -0.125 to 0.125
- w_key: bfloat16 [2048, 128], replicated, may hold values from -0.125 to 0.125
- w_value: bfloat16 [2048, 128], replicated, may hold values from -0.125 to 0.125
- query_gain: float32 [64], replicated, may hold values from 0.5 to 10
- key_gain: float32 [64], replicated, may hold values from 0.5 to 10
- sink_logit: float32 [16], P('tp'), may hold values from 1 to 5
- w_output: bfloat16 [1024, 2048], P('tp'), may hold values from -0.1875 to 0.1875
- expert_input: bfloat16 [1024, 2048], P('ep'), may hold values from -6 to 6
- expert_gain: float32 [2048], replicated, may hold values from 0.1 to 1.9
- route_ids: int32 [1024, 4], P('ep'), may hold values from 0 to 7, all different within a row; in each aligned block of 128 rows (0 to 127, 128 to 255, ...) at most 128 rows name the same one
- route_weight: float32 [1024, 4], P('ep'), may hold values from 0.2 to 1.2
- expert_gate: bfloat16 [8, 2048, 2048], P('ep', None, 'tp'), may hold values from -0.125 to 0.125
- expert_up: bfloat16 [8, 2048, 2048], P('ep', None, 'tp'), may hold values from -0.125 to 0.125
- expert_down: bfloat16 [8, 2048, 2048], P('ep', None, 'tp'), may hold values from -0.125 to 0.125
- shared_gate: bfloat16 [2048, 1024], P(None, 'tp'), may hold values from -0.125 to 0.125
- shared_up: bfloat16 [2048, 1024], P(None, 'tp'), may hold values from -0.125 to 0.125
- shared_down: bfloat16 [1024, 2048], P(None, 'tp'), may hold values from -0.1875 to 0.1875
Outputs:
- mixer_output: bfloat16 [4096, 2048], P('ep', 'tp')
- expert_output: bfloat16 [1024, 2048], P('ep', 'tp')
The draws below stay inside these ranges and needn't reach their ends.
Inputs may be any that keep to these rules, and one draw needn't show every extreme that they name: `route_ids`: each row names 4 different experts. In the rows of one index of ep (aligned blocks of 128 rows) no expert is named by more than 128 rows, a bound that some block reaches.
All inputs are finite; a program needn't handle non-finite values.
Results may differ from the reference program's by a relative error of at most 0.018.
The reference program's roundings to bfloat16 on the way count: a program that leaves them out, or rounds other values in their place, can miss the bound.
Values may be sent and summed in bfloat16 or wider, within the bound.
No kernel may reach another device: no remote copies, remote signals or barrier semaphores. Data moves between devices by JAX's collectives and lax.ppermute only.
A program may use at most 64 MiB of HBM per device.

```python
import math
import jax
import jax.numpy as jnp
import numpy as np
from jax import lax

D = 2048
HEAD = 64
Q_HEADS = 16
KV_HEADS = 2
WINDOW = 128
TOK_B = 128
TOPK = 4
FF = 2048
SHARED_FF = 1024
EXPERTS = 8
CAP = 128
TOKENS_A = 4096
TOKENS_B = 1024
N_EP = 8


def gain_draw(key):
    return jax.random.uniform(key, (HEAD,), jnp.float32, 0.6, 1.6)


def draw_query_gain(key, part):
    return gain_draw(jax.random.fold_in(key, 11))


def draw_key_gain(key, part):
    return gain_draw(jax.random.fold_in(key, 23))


def level_of(rng, extent, shards, low, largest):
    loudness = 1.0
    for position, shards_of in shards:
        steps = jax.random.uniform(jax.random.fold_in(jax.random.fold_in(rng, 6), position), (shards_of,), jnp.float32, low / len(shards), largest / len(shards))
        loudness = loudness * jnp.repeat(jnp.exp(steps), extent[position] // shards_of).reshape((-1,) + (1,) * (len(extent) - 1 - position))
    return loudness


def deal_out(stream_key, own, number, rows, count, top, most, skew):
    ranking = jax.random.permutation(stream_key, count)
    heavy_load, ordinary = portions_of(count, rows * top, most, skew, True), portions_of(count, rows * top, most, skew, False)
    places = jnp.arange(count)

    def named(sizes, rotation):
        used = int((sizes > 0).sum())
        fixed = max(1, used // 4)
        shifted = fixed + (places - fixed + rotation * (used - fixed)) % max(1, count - fixed)
        return jnp.zeros((count,), jnp.int32).at[ranking[jnp.where(places < fixed, places, shifted)]].set(jnp.asarray(sizes, jnp.int32))

    sizes = jnp.where(number % 4 == 0, named(heavy_load, number // 4), named(ordinary, number - number // 4 - 1))
    mixed = jax.random.permutation(jax.random.fold_in(own, 3), count)
    donor, taker = mixed[0:count // 2 * 2:2], mixed[1:count // 2 * 2:2]
    room = jnp.minimum(sizes[donor] - 1, most - sizes[taker]) // 2
    room = jnp.where((donor == ranking[0]) | (taker == ranking[0]) | (sizes[taker] == 0), 0, jnp.maximum(room, 0))
    shifted = jax.random.randint(jax.random.fold_in(own, 4), (count // 2,), 0, 1 << 20) % (room + 1)
    sizes = sizes.at[donor].add(-shifted).at[taker].add(shifted)
    items = jnp.searchsorted(jnp.cumsum(sizes), jnp.arange(rows * top), side="right").astype(jnp.int32)
    listing = items.reshape(top, rows).T
    listing = listing[jax.random.permutation(jax.random.fold_in(own, 1), rows)]
    rotation = jax.random.randint(jax.random.fold_in(own, 2), (rows, 1), 0, top)
    return jnp.take_along_axis(listing, (jnp.arange(top)[None, :] + rotation) % top, axis=1)


def portions_of(count, total, limit, skew, full):
    loads = [(1 << 20) // math.isqrt(grade ** skew) + 1 for grade in range(1, count + 1)]
    largest = limit if full else min(limit, max(-(-total // count), total * loads[0] // sum(loads)))
    least = 1 if total - largest >= count - 1 else 0
    holding, spare = [largest] + [least] * (count - 1), total - largest - least * (count - 1)
    while spare > 0:
        movable = [i for i in range(1, count) if holding[i] < largest] or [i for i in range(1, count) if holding[i] < limit]
        mass, remaining = sum([loads[i] for i in movable]), spare
        for i in movable:
            more = min(limit - holding[i], max(1, remaining * loads[i] // mass), spare)
            holding[i] = holding[i] + more
            spare = spare - more
    return np.array(holding)


def centred(stream_key, extent, width, bound, split=(), kind=jnp.bfloat16):
    array = jax.random.normal(stream_key, extent, jnp.float32) * width
    if len(split) > 0:
        array = level_of(stream_key, extent, split, -0.22, 0.18) * array
    return jnp.clip(array, min=-bound, max=bound).astype(kind)


def setup_inputs(seed: int = 0) -> dict:
    streams_of = jax.random.split(jax.random.key(seed), 20)
    mixer_input = centred(streams_of[0], (TOKENS_A, D), 1.0, 6.0, ((0, 8), (1, 4)))
    mixer_gain = jnp.clip(1.0 + 0.18 * jax.random.normal(streams_of[1], (D,), jnp.float32), 0.1, 1.9)
    w_query = centred(streams_of[2], (D, Q_HEADS * HEAD), D ** -0.5, 0.125, ((1, 4),))
    w_key = centred(streams_of[3], (D, KV_HEADS * HEAD), D ** -0.5, 0.125)
    w_value = centred(streams_of[4], (D, KV_HEADS * HEAD), D ** -0.5, 0.125)
    query_gain = draw_query_gain(jax.random.fold_in(streams_of[19], 71), 0)
    key_gain = draw_key_gain(jax.random.fold_in(streams_of[19], 71), 0)
    sink_logit = jnp.clip(1.0 + 4.0 * jax.random.uniform(streams_of[7], (Q_HEADS,), jnp.float32) ** level_of(streams_of[7], (Q_HEADS,), ((0, 4),), -0.2, 0.2), 1.0, 5.0)
    w_output = centred(streams_of[8], (Q_HEADS * HEAD, D), (Q_HEADS * HEAD) ** -0.5, 0.1875, ((0, 4),))
    expert_input = centred(streams_of[9], (TOKENS_B, D), 1.0, 6.0, ((0, 8),))
    expert_gain = jnp.clip(1.0 + 0.18 * jax.random.normal(streams_of[10], (D,), jnp.float32), 0.1, 1.9)
    route_ids_keys = jax.random.split(jax.random.fold_in(streams_of[11], 1), TOKENS_B // TOK_B)
    route_ids_turns = jax.random.permutation(jax.random.fold_in(streams_of[11], 3), TOKENS_B // TOK_B)
    route_ids = jax.vmap(lambda own, number: deal_out(jax.random.fold_in(streams_of[11], 2), own, number, TOK_B, EXPERTS, TOPK, CAP, 1))(route_ids_keys, route_ids_turns).reshape((TOKENS_B, TOPK))
    route_weight = jnp.clip(0.2 + 1 * jax.random.uniform(streams_of[12], (TOKENS_B, TOPK), jnp.float32) ** level_of(streams_of[12], (TOKENS_B, TOPK), ((0, 8),), -0.2, 0.2), 0.2, 1.2)
    expert_gate = centred(streams_of[13], (EXPERTS, D, FF), D ** -0.5, 0.125, ((0, 8), (2, 4)))
    expert_up = centred(streams_of[14], (EXPERTS, D, FF), D ** -0.5, 0.125, ((0, 8), (2, 4)))
    expert_down = centred(streams_of[15], (EXPERTS, FF, D), FF ** -0.5, 0.125, ((0, 8), (2, 4)))
    shared_gate = centred(streams_of[16], (D, SHARED_FF), D ** -0.5, 0.125, ((1, 4),))
    shared_up = centred(streams_of[17], (D, SHARED_FF), D ** -0.5, 0.125, ((1, 4),))
    shared_down = centred(streams_of[18], (SHARED_FF, D), SHARED_FF ** -0.5, 0.1875, ((1, 4),))
    return dict(mixer_input=mixer_input, mixer_gain=mixer_gain, w_query=w_query, w_key=w_key, w_value=w_value, query_gain=query_gain, key_gain=key_gain, sink_logit=sink_logit, w_output=w_output, expert_input=expert_input, expert_gain=expert_gain, route_ids=route_ids, route_weight=route_weight, expert_gate=expert_gate, expert_up=expert_up, expert_down=expert_down, shared_gate=shared_gate, shared_up=shared_up, shared_down=shared_down)


EPSILON = 1e-06

def head_norm(matrix, gain_vector):
    return matrix * lax.rsqrt(lax.optimization_barrier(jnp.mean(matrix * matrix, axis=-1, keepdims=True)) + EPSILON) * gain_vector

def band_attend(queries, keys_own, values_own, keys_prev, values_prev, sink_logit, first_row):
    row_count = queries.shape[0]
    head_count = queries.shape[1]
    blocks = row_count // WINDOW
    keys_all = jnp.concatenate([keys_prev, keys_own], axis=0)
    values_all = jnp.concatenate([values_prev, values_own], axis=0)
    key_band = jnp.concatenate([keys_all[:row_count].reshape(blocks, WINDOW, HEAD), keys_own.reshape(blocks, WINDOW, HEAD)], axis=1)
    value_band = jnp.concatenate([values_all[:row_count].reshape(blocks, WINDOW, HEAD), values_own.reshape(blocks, WINDOW, HEAD)], axis=1)
    query_blocks = queries.reshape(blocks, WINDOW, head_count, HEAD)
    scores = jnp.einsum('nqhd,nkd->nhqk', query_blocks.astype(jnp.float32), key_band.astype(jnp.float32)) * HEAD ** (-0.5)
    query_idx = jnp.arange(WINDOW, dtype=jnp.int32)[:, None]
    key_idx = jnp.arange(2 * WINDOW, dtype=jnp.int32)[None, :]
    relative = query_idx + WINDOW - key_idx
    block_idx = jnp.arange(blocks, dtype=jnp.int32)[:, None, None]
    key_pos = first_row + block_idx * WINDOW - WINDOW + key_idx[None]
    allowed = ((relative >= 0) & (relative < WINDOW))[None] & (key_pos >= 0)
    allowed = allowed[:, None]
    masked = jnp.where(allowed, scores, -jnp.inf)
    sink_column = sink_logit.astype(jnp.float32).reshape(1, head_count, 1, 1)
    peak_score = jnp.maximum(lax.optimization_barrier(jnp.max(masked, axis=-1, keepdims=True)), sink_column)
    exponent = jnp.exp(masked - peak_score)
    denominator = lax.optimization_barrier(jnp.sum(exponent, axis=-1, keepdims=True)) + jnp.exp(sink_column - peak_score)
    probability = (exponent / denominator).astype(jnp.bfloat16)
    mixed_rows = jnp.einsum('nhqk,nkd->nqhd', probability.astype(jnp.float32), value_band.astype(jnp.float32))
    return mixed_rows.reshape(row_count, head_count * HEAD).astype(jnp.bfloat16)

def reference(mixer_input, mixer_gain, w_query, w_key, w_value, query_gain, key_gain, sink_logit, w_output, expert_input, expert_gain, route_ids, route_weight, expert_gate, expert_up, expert_down, shared_gate, shared_up, shared_down):
    rows_float = mixer_input.astype(jnp.float32)
    scaled = (rows_float * mixer_gain).astype(jnp.bfloat16)
    inv_rms = lax.rsqrt(lax.optimization_barrier(jnp.mean(rows_float * rows_float, axis=-1, keepdims=True)) + EPSILON)
    query_raw = jnp.dot(scaled, w_query, preferred_element_type=jnp.float32)
    key_raw = jnp.dot(scaled, w_key, preferred_element_type=jnp.float32)
    value_raw = jnp.dot(scaled, w_value, preferred_element_type=jnp.float32)
    queries = head_norm(query_raw.reshape(TOKENS_A, Q_HEADS, HEAD), query_gain).astype(jnp.bfloat16)
    keys_all = head_norm(key_raw.reshape(TOKENS_A, KV_HEADS, HEAD), key_gain).astype(jnp.bfloat16)
    values_all = (value_raw * inv_rms).astype(jnp.bfloat16).reshape(TOKENS_A, KV_HEADS, HEAD)
    group_size = Q_HEADS // KV_HEADS
    zero_rows = jnp.zeros((WINDOW, HEAD), jnp.bfloat16)

    def one_head(head_index):
        kv_index = head_index // group_size
        head_query = queries[:, head_index][:, None, :]
        head_keys = keys_all[:, kv_index]
        head_values = values_all[:, kv_index]
        sink_one = sink_logit[head_index].reshape(1)
        return band_attend(head_query, head_keys, head_values, zero_rows, zero_rows, sink_one, jnp.int32(0))
    per_head = lax.map(one_head, jnp.arange(Q_HEADS, dtype=jnp.int32))
    attended = jnp.transpose(per_head, (1, 0, 2)).reshape(TOKENS_A, Q_HEADS * HEAD)
    mixer_output = jnp.dot(attended, w_output, preferred_element_type=jnp.float32).astype(jnp.bfloat16)
    expert_float = expert_input.astype(jnp.float32)
    normed = (expert_float * lax.rsqrt(lax.optimization_barrier(jnp.mean(expert_float * expert_float, axis=-1, keepdims=True)) + EPSILON) * expert_gain).astype(jnp.bfloat16)
    shared_hidden = (jax.nn.silu(jnp.dot(normed, shared_gate, preferred_element_type=jnp.float32)) * jnp.dot(normed, shared_up, preferred_element_type=jnp.float32)).astype(jnp.bfloat16)
    shared_out = jnp.dot(shared_hidden, shared_down, preferred_element_type=jnp.float32)
    ids_blocks = route_ids.reshape(N_EP, TOK_B * TOPK)
    onehot = (ids_blocks[:, :, None] == jnp.arange(EXPERTS, dtype=jnp.int32)[None, None, :]).astype(jnp.int32)
    earlier = jnp.cumsum(onehot, axis=1) - onehot
    slot_index = lax.optimization_barrier(jnp.sum(earlier * onehot, axis=-1))
    block_ids = jnp.arange(N_EP, dtype=jnp.int32)[:, None]
    slot_column = (block_ids * CAP + slot_index).astype(jnp.int32)
    token_ids = (block_ids * TOK_B + jnp.arange(TOK_B * TOPK, dtype=jnp.int32)[None] // TOPK).astype(jnp.int32)
    slot_table = jnp.full((EXPERTS, N_EP * CAP), TOKENS_B, jnp.int32).at[ids_blocks, slot_column].set(token_ids)
    padded = jnp.concatenate([normed, jnp.zeros((1, D), jnp.bfloat16)], axis=0)

    def one_expert(expert_index):
        chosen = padded[slot_table[expert_index]]
        gate_pre = jnp.dot(chosen, expert_gate[expert_index], preferred_element_type=jnp.float32)
        up_pre = jnp.dot(chosen, expert_up[expert_index], preferred_element_type=jnp.float32)
        hidden = (jax.nn.silu(gate_pre) * up_pre).astype(jnp.bfloat16)
        return jnp.dot(hidden, expert_down[expert_index], preferred_element_type=jnp.float32).astype(jnp.bfloat16)
    routed = lax.map(one_expert, jnp.arange(EXPERTS, dtype=jnp.int32))
    picked = routed[ids_blocks, slot_column].reshape(TOKENS_B, TOPK, D).astype(jnp.float32)
    expert_output = (shared_out + lax.optimization_barrier(jnp.sum(picked * route_weight[:, :, None], axis=1))).astype(jnp.bfloat16)
    return (mixer_output, expert_output)
```

```python
import functools

import jax
import jax.numpy as jnp
from jax import lax
from jax.experimental import pallas as pl
from jax.experimental.pallas import tpu as pltpu
from jax.sharding import PartitionSpec as P

HEAD = 64
KV_HEADS = 2
WINDOW = 128
CORES = 2
EPSILON = 1e-06
MIB = 1 << 20


def dot(left, right):
    return jnp.dot(left, right, preferred_element_type=jnp.float32)


def pick(blocks, index):
    chosen = blocks[0]
    for number in range(1, len(blocks)):
        chosen = jnp.where(index == number, blocks[number], chosen)
    return chosen


def kernel_call(body, outs, args, flops, mib=16, scratch=()):
    values, specs = [], []
    for arg in args:
        space, value = arg if isinstance(arg, tuple) else ("hbm", arg)
        if space == "vmem":
            values.append(pltpu.with_memory_space_constraint(value, pltpu.VMEM))
            specs.append(pl.BlockSpec(memory_space=pltpu.VMEM))
        elif space == "smem":
            values.append(value)
            specs.append(pl.BlockSpec(memory_space=pltpu.SMEM))
        elif space == "any":
            values.append(pltpu.with_memory_space_constraint(value, pltpu.HBM))
            specs.append(pl.BlockSpec(memory_space=pltpu.HBM))
        else:
            values.append(pltpu.with_memory_space_constraint(value, pltpu.HBM))
            specs.append(pl.BlockSpec())
    single = not isinstance(outs, list)
    return pl.pallas_call(
        body,
        out_shape=outs,
        in_specs=specs,
        out_specs=out_spec(outs) if single else [out_spec(out) for out in outs],
        scratch_shapes=list(scratch),
        compiler_params=pltpu.CompilerParams(vmem_limit_bytes=mib * MIB),
        cost_estimate=pl.CostEstimate(flops=flops, bytes_accessed=0, transcendentals=0),
    )(*values)


def out_spec(out):
    if isinstance(out, jax.ShapeDtypeStruct):
        return pl.BlockSpec()
    return pl.BlockSpec(memory_space=pltpu.VMEM)


def vmem(arrays):
    return [("vmem", array) for array in arrays]


def load_body(*refs):
    count = len(refs) // 3
    copies = [
        pltpu.make_async_copy(refs[i], refs[count + i], refs[2 * count + i]) for i in range(count)
    ]
    for copy in copies:
        copy.start()
    for copy in copies:
        copy.wait()


def core_now():
    return lax.rem(lax.axis_index("tp"), CORES)


def norm_body(x_ref, gain_ref, ids_ref, route_ref, normed_ref, half_ref, rest_ref, info_ref):
    value = x_ref[...].astype(jnp.float32)
    scale = lax.rsqrt(jnp.mean(value * value, axis=-1, keepdims=True) + EPSILON)
    normed = (value * scale * gain_ref[...]).astype(jnp.bfloat16)
    normed_ref[...] = normed
    half = half_ref.shape[1]
    low, high, first = normed[:, :half], normed[:, half:], core_now() == 0
    half_ref[...] = jnp.where(first, low, high)
    rest_ref[...] = jnp.where(first, high, low)
    both = jnp.concatenate([ids_ref[...].astype(jnp.float32), route_ref[...]], axis=0)
    info_ref[...] = both.T


def silu_product(gate, up):
    return (jax.nn.silu(gate) * up).astype(jnp.bfloat16)


def shared_body(normed_ref, gate_ref, up_ref, out_ref):
    normed = normed_ref[...]
    out_ref[...] = silu_product(dot(normed, gate_ref[...]), dot(normed, up_ref[...]))


def hidden_body(count, *refs):
    own, other = refs[:count], refs[count : 2 * count]
    gate_ref, up_ref, out_ref = refs[2 * count :]
    half = own[0].shape[1]
    core = core_now()
    low = pl.ds(pl.multiple_of(core * half, half), half)
    high = pl.ds(pl.multiple_of((1 - core) * half, half), half)
    mine = jnp.concatenate([ref[...] for ref in own], axis=0)
    theirs = jnp.concatenate([ref[...] for ref in other], axis=0)
    gate = dot(mine, gate_ref[0, low, :]) + dot(theirs, gate_ref[0, high, :])
    up = dot(mine, up_ref[0, low, :]) + dot(theirs, up_ref[0, high, :])
    out_ref[...] = silu_product(gate, up)


def quarter_slices(y_count, size):
    index = lax.axis_index("tp")
    y, core = lax.div(index, CORES), lax.rem(index, CORES)
    slices = []
    for side in (core, 1 - core):
        for k in range(y_count):
            start = (lax.rem(y + y_count - k, y_count) * CORES + side) * size
            slices.append(pl.ds(pl.multiple_of(start, size), size))
    return slices


def gathered_dot(refs, weight, y_count):
    width = refs[0].shape[1]
    total = None
    for ref, rows in zip(refs, quarter_slices(y_count, width)):
        part = dot(ref[...], weight[rows, :])
        total = part if total is None else total + part
    return total


def down_body(y_count, *refs):
    pieces = refs[: CORES * y_count]
    weight_ref, outs = refs[CORES * y_count], refs[CORES * y_count + 1 :]
    total = gathered_dot(pieces, weight_ref.at[0], y_count)
    outs[0][...] = total.astype(jnp.bfloat16)


def weighted_rows(blocks, info_ref, r, z_count, x_count):
    index = lax.axis_index("ep")
    z, x = lax.div(index, x_count), lax.rem(index, x_count)
    info = info_ref[...]
    tokens, topk = info.shape[0], info.shape[1] // 2
    total = None
    for s, block in enumerate(blocks):
        expert = (lax.rem(z + s, z_count) * x_count + x).astype(jnp.float32)
        chosen = jnp.where(info[:, :topk] == expert, info[:, topk:], 0.0)
        weight = jnp.sum(chosen, axis=1, keepdims=True)
        part = block[r * tokens : (r + 1) * tokens, :].astype(jnp.float32) * weight
        total = part if total is None else total + part
    return total


def partial_body(z_count, x_count, *refs):
    blocks, infos, outs = refs[:z_count], refs[z_count : z_count + x_count - 1], None
    outs = refs[z_count + x_count - 1 :]
    for r, (info, out) in enumerate(zip(infos, outs), 1):
        out[...] = weighted_rows(blocks, info, r, z_count, x_count).astype(jnp.bfloat16)


def base_body(y_count, z_count, x_count, *refs):
    pieces, blocks = refs[: CORES * y_count], refs[CORES * y_count : CORES * y_count + z_count]
    weight_ref, info_ref, out_ref = refs[CORES * y_count + z_count :]
    total = gathered_dot(pieces, weight_ref, y_count)
    out_ref[...] = total + weighted_rows(blocks, info_ref, 0, z_count, x_count)


def merge_body(y_count, *refs):
    keeps, taken_ref = refs[:y_count], refs[y_count]
    total_ref, sends = refs[y_count + 1], refs[y_count + 2 :]
    for k, send in enumerate(sends, 1):
        send[...] = (keeps[k][...] + taken_ref[k].astype(jnp.float32)).astype(jnp.bfloat16)
    total_ref[...] = keeps[0][...] + taken_ref[0].astype(jnp.float32)


def finish_body(*refs):
    total = refs[0][...]
    for ref in refs[1:-1]:
        total = total + ref[...].astype(jnp.float32)
    refs[-1][...] = total.astype(jnp.bfloat16)


def project_body(y_count, *refs):
    pieces = refs[: CORES * y_count]
    gain_ref, wq_ref, wk_ref, wv_ref, qg_ref, kg_ref, q_ref, kv_ref = refs[CORES * y_count :]
    _, width = pieces[0].shape
    index = lax.axis_index("tp")
    y, core = lax.div(index, CORES), lax.rem(index, CORES)
    query = key = value = squares = None
    number = 0
    for side in (core, 1 - core):
        for k in range(y_count):
            quarter = lax.rem(y + y_count - k, y_count) * CORES + side
            at = pl.ds(pl.multiple_of(quarter * width, width), width)
            x = pieces[number][...].astype(jnp.float32)
            scaled = (x * gain_ref[:, at]).astype(jnp.bfloat16)
            parts = [
                dot(scaled, wq_ref[at, :]),
                dot(scaled, wk_ref[at, :]),
                dot(scaled, wv_ref[at, :]),
                jnp.sum(x * x, axis=1, keepdims=True),
            ]
            if number == 0:
                query, key, value, squares = parts
            else:
                query, key, value, squares = (
                    query + parts[0],
                    key + parts[1],
                    value + parts[2],
                    squares + parts[3],
                )
            number += 1
    inv_rms = lax.rsqrt(squares / (number * width) + EPSILON)
    head_of = lax.broadcasted_iota(jnp.int32, query.shape, 1) // HEAD
    query_squares = query * query
    scale = jnp.zeros_like(query)
    for h in range(query.shape[1] // HEAD):
        mean = jnp.sum(jnp.where(head_of == h, query_squares, 0.0), axis=1, keepdims=True) / HEAD
        scale = jnp.where(head_of == h, lax.rsqrt(mean + EPSILON), scale)
    query_gain = jnp.concatenate([qg_ref[...]] * (query.shape[1] // HEAD), axis=1)
    q_ref[...] = (query * scale * query_gain).astype(jnp.bfloat16)
    kv_index = lax.div(index, lax.axis_size("tp") // KV_HEADS)
    keys = pick([key[:, i * HEAD : (i + 1) * HEAD] for i in range(KV_HEADS)], kv_index)
    values = pick([value[:, i * HEAD : (i + 1) * HEAD] for i in range(KV_HEADS)], kv_index)
    mean = jnp.mean(keys * keys, axis=1, keepdims=True)
    keys = (keys * lax.rsqrt(mean + EPSILON) * kg_ref[...]).astype(jnp.bfloat16)
    kv_ref[...] = jnp.concatenate([keys, (values * inv_rms).astype(jnp.bfloat16)], axis=1)


def attend_body(y_count, q_ref, kv_ref, prev_ref, sink_ref, wo_ref, *outs):
    gives, keeps = outs[0], outs[1:]
    rows, columns = q_ref.shape
    heads = columns // HEAD
    first_row = lax.axis_index("ep") * rows
    head_of = lax.broadcasted_iota(jnp.int32, (WINDOW, columns), 1) // HEAD
    query_at = lax.broadcasted_iota(jnp.int32, (WINDOW, 2 * WINDOW), 0)
    key_at = lax.broadcasted_iota(jnp.int32, (WINDOW, 2 * WINDOW), 1)
    relative = query_at + WINDOW - key_at
    band = (relative >= 0) & (relative < WINDOW)
    head_row = lax.broadcasted_iota(jnp.int32, (heads * WINDOW, 1), 0) // WINDOW
    sink = jnp.zeros((heads * WINDOW, 1), jnp.float32)
    for h in range(heads):
        sink = jnp.where(head_row == h, sink_ref[h], sink)
    attended = []
    for block in range(rows // WINDOW):
        at = block * WINDOW
        own = kv_ref[at : at + WINDOW, :]
        prev = prev_ref[...] if block == 0 else kv_ref[at - WINDOW : at, :]
        both = jnp.concatenate([prev, own], axis=0)
        keys = jnp.concatenate([both[:, :HEAD]] * heads, axis=1)
        values = jnp.concatenate([both[:, HEAD:]] * heads, axis=1)
        queries = q_ref[at : at + WINDOW, :]
        allowed = band & (first_row + at - WINDOW + key_at >= 0)
        allowed = jnp.concatenate([allowed] * heads, axis=0)
        nothing = jnp.zeros_like(queries)
        masked = [jnp.where(head_of == h, queries, nothing) for h in range(heads)]
        scores = lax.dot_general(
            jnp.concatenate(masked, axis=0),
            keys,
            (((1,), (1,)), ((), ())),
            preferred_element_type=jnp.float32,
        ) * HEAD ** (-0.5)
        scores = jnp.where(allowed, scores, -jnp.inf)
        peak = jnp.maximum(jnp.max(scores, axis=1, keepdims=True), sink)
        exponent = jnp.exp(scores - peak)
        total = jnp.sum(exponent, axis=1, keepdims=True) + jnp.exp(sink - peak)
        probability = (exponent / total).astype(jnp.bfloat16)
        spread = dot(probability, values)
        mixed = jnp.zeros((WINDOW, columns), jnp.float32)
        for h in range(heads):
            mixed = jnp.where(head_of == h, spread[h * WINDOW : (h + 1) * WINDOW], mixed)
        attended.append(mixed.astype(jnp.bfloat16))
    attended = jnp.concatenate(attended, axis=0)
    index = lax.axis_index("tp")
    y, core = lax.div(index, CORES), lax.rem(index, CORES)
    width = gives.shape[2]
    for k in range(y_count):
        base = lax.rem(y + k, y_count) * CORES
        at = pl.ds(pl.multiple_of((base + 1 - core) * width, width), width)
        gives[k] = dot(attended, wo_ref[:, at]).astype(jnp.bfloat16)
    for k in range(y_count):
        base = lax.rem(y + k, y_count) * CORES
        at = pl.ds(pl.multiple_of((base + core) * width, width), width)
        keeps[k][...] = dot(attended, wo_ref[:, at])


def shards(
    mixer_input,
    mixer_gain,
    w_query,
    w_key,
    w_value,
    query_gain,
    key_gain,
    sink_logit,
    w_output,
    expert_input,
    expert_gain,
    route_ids,
    route_weight,
    expert_gate,
    expert_up,
    expert_down,
    shared_gate,
    shared_up,
    shared_down,
):
    tp_count = lax.axis_size("tp")
    ep_count = lax.axis_size("ep")
    y_count = tp_count // CORES
    x_count = 1 << ((ep_count.bit_length() - 1) // 2)
    z_count = ep_count // x_count
    bf16, f32 = jnp.bfloat16, jnp.float32
    shape = pltpu.VMEM
    final = jax.ShapeDtypeStruct

    def across(value):
        return lax.ppermute(value, "tp", [(t, t ^ 1) for t in range(tp_count)])

    def turn_y(value, step):
        pairs = [
            (y * CORES + c, (y + step) % y_count * CORES + c)
            for y in range(y_count)
            for c in range(CORES)
        ]
        return lax.ppermute(value, "tp", pairs)

    def turn_ep(value, z_step, x_step):
        pairs = [
            (z * x_count + x, (z + z_step) % z_count * x_count + (x + x_step) % x_count)
            for z in range(z_count)
            for x in range(x_count)
        ]
        return lax.ppermute(value, "ep", pairs)

    def gather_tp(value):
        turned = [value] + [turn_y(value, k) for k in range(1, y_count)]
        return turned + [across(v) for v in turned]

    tokens, width = expert_input.shape
    half = width // CORES
    rows = mixer_input.shape[0]
    piece = width // tp_count
    columns = w_query.shape[1]
    hidden_width = expert_gate.shape[2]
    out_width = expert_down.shape[2]

    mixer_pieces = gather_tp(mixer_input)
    normed, own_half, own_rest, info = kernel_call(
        norm_body,
        [shape((tokens, width), bf16)]
        + [shape((tokens, half), bf16)] * 2
        + [shape((tokens, 2 * route_ids.shape[1]), f32)],
        [expert_input, expert_gain.reshape(1, width), route_ids.T, route_weight.T],
        8 * tokens * width,
        8,
    )
    z_blocks = [own_half] + [turn_ep(own_half, s, 0) for s in range(1, z_count)]
    blocks = []
    for s in range(z_count):
        blocks.append([z_blocks[s]] + [turn_ep(z_blocks[s], 0, r) for r in range(1, x_count)])
    others = [
        [across(block) if s or r else own_rest for r, block in enumerate(blocks[s])]
        for s in range(z_count)
    ]

    def load(weights):
        return kernel_call(
            load_body,
            [shape(weight.shape, bf16) for weight in weights],
            [("any", weight) for weight in weights],
            1000,
            8,
            [pltpu.SemaphoreType.DMA] * len(weights),
        )

    gate, up, down = load([expert_gate, expert_up, expert_down])
    late = load([w_query, w_key, w_value, w_output, shared_down])
    w_query, w_key, w_value, w_output, shared_down = late
    shared_hidden = kernel_call(
        shared_body,
        shape((tokens, shared_gate.shape[1]), bf16),
        [("vmem", normed), shared_gate, shared_up],
        4 * tokens * width * shared_gate.shape[1],
    )
    infos = [info] + [turn_ep(info, 0, r) for r in range(1, x_count)]
    shared_pieces = gather_tp(shared_hidden)

    queries, keys_values = kernel_call(
        functools.partial(project_body, y_count),
        [shape((rows, columns), bf16), shape((rows, 2 * HEAD), bf16)],
        [mixer_pieces[0]]
        + vmem(mixer_pieces[1:])
        + [mixer_gain.reshape(1, width)]
        + vmem([w_query, w_key, w_value])
        + [
            query_gain.reshape(1, HEAD),
            key_gain.reshape(1, HEAD),
        ],
        2 * rows * width * (columns + 4 * HEAD),
    )
    before = lax.ppermute(
        keys_values[rows - WINDOW :], "ep", [(i, i + 1) for i in range(ep_count - 1)]
    )
    attended = kernel_call(
        functools.partial(attend_body, y_count),
        [shape((y_count, rows, piece), bf16)] + [shape((rows, piece), f32)] * y_count,
        vmem([queries, keys_values, before]) + [("smem", sink_logit), ("vmem", w_output)],
        2 * rows * columns * width,
    )
    taken = across(attended[0])
    merged = kernel_call(
        functools.partial(merge_body, y_count),
        [shape((rows, piece), f32)] + [shape((rows, piece), bf16)] * (y_count - 1),
        vmem([*attended[1:], taken]),
        rows * width,
    )
    received = [turn_y(sent, k) for k, sent in enumerate(merged[1:], 1)]
    mixer_output = kernel_call(
        finish_body, final((rows, piece), bf16), vmem([merged[0], *received]), rows * width
    )

    returned = []
    for s in range(z_count):
        hidden = kernel_call(
            functools.partial(hidden_body, x_count),
            shape((x_count * tokens, hidden_width), bf16),
            vmem(blocks[s] + others[s] + [gate, up]),
            4 * x_count * tokens * width * hidden_width,
        )
        routed = kernel_call(
            functools.partial(down_body, y_count),
            shape((x_count * tokens, out_width), bf16),
            vmem(gather_tp(hidden) + [down]),
            2 * x_count * tokens * expert_down.shape[1] * out_width,
        )
        returned.append(turn_ep(routed, -s, 0) if s else routed)
    partials = kernel_call(
        functools.partial(partial_body, z_count, x_count),
        [shape((tokens, out_width), bf16)] * (x_count - 1),
        vmem(returned + infos[1:]),
        2 * tokens * out_width * ep_count,
    )
    crossed = [turn_ep(part, 0, -r) for r, part in enumerate(partials, 1)]
    base = kernel_call(
        functools.partial(base_body, y_count, z_count, x_count),
        shape((tokens, out_width), f32),
        vmem(shared_pieces + returned + [shared_down, info]),
        2 * tokens * shared_down.shape[0] * out_width,
    )
    expert_output = kernel_call(
        finish_body, final((tokens, out_width), bf16), vmem([base] + crossed), tokens * out_width
    )
    return (mixer_output, expert_output)


def solution(mesh):
    in_specs = (
        P("ep", "tp"),
        P(),
        P(None, "tp"),
        P(),
        P(),
        P(),
        P(),
        P("tp"),
        P("tp", None),
        P("ep", None),
        P(),
        P("ep", None),
        P("ep", None),
        P("ep", None, "tp"),
        P("ep", None, "tp"),
        P("ep", None, "tp"),
        P(None, "tp"),
        P(None, "tp"),
        P(None, "tp"),
    )
    out_specs = (P("ep", "tp"), P("ep", "tp"))

    return jax.shard_map(shards, mesh=mesh, in_specs=in_specs, out_specs=out_specs, check_vma=False)
```

```python
import functools

import jax
import jax.numpy as jnp
from jax import lax
from jax.experimental import pallas as pl
from jax.experimental.pallas import tpu as pltpu
from jax.sharding import PartitionSpec as P

HEAD = 64
KV_HEADS = 2
WINDOW = 128
CORES = 2
SUBLANES = 8
EPSILON = 1e-06
MIB = 1 << 20


def dot(left, right):
    return jnp.dot(left, right, preferred_element_type=jnp.float32)


def pick(blocks, index):
    chosen = blocks[0]
    for number in range(1, len(blocks)):
        chosen = jnp.where(index == number, blocks[number], chosen)
    return chosen


def kernel_call(body, outs, args, flops, mib=16, scratch=()):
    values, specs = [], []
    for arg in args:
        space, value = arg if isinstance(arg, tuple) else ("hbm", arg)
        if space == "vmem":
            values.append(pltpu.with_memory_space_constraint(value, pltpu.VMEM))
            specs.append(pl.BlockSpec(memory_space=pltpu.VMEM))
        elif space == "smem":
            values.append(value)
            specs.append(pl.BlockSpec(memory_space=pltpu.SMEM))
        elif space == "any":
            values.append(pltpu.with_memory_space_constraint(value, pltpu.HBM))
            specs.append(pl.BlockSpec(memory_space=pltpu.HBM))
        else:
            values.append(pltpu.with_memory_space_constraint(value, pltpu.HBM))
            specs.append(pl.BlockSpec())
    single = not isinstance(outs, list)
    return pl.pallas_call(
        body,
        out_shape=outs,
        in_specs=specs,
        out_specs=out_spec(outs) if single else [out_spec(out) for out in outs],
        scratch_shapes=list(scratch),
        compiler_params=pltpu.CompilerParams(vmem_limit_bytes=mib * MIB),
        cost_estimate=pl.CostEstimate(flops=flops, bytes_accessed=0, transcendentals=0),
    )(*values)


def out_spec(out):
    if isinstance(out, jax.ShapeDtypeStruct):
        return pl.BlockSpec()
    return pl.BlockSpec(memory_space=pltpu.VMEM)


def vmem(arrays):
    return [("vmem", array) for array in arrays]


def start_loads(sources, targets, semaphores):
    copies = [
        pltpu.make_async_copy(source, target, semaphore)
        for source, target, semaphore in zip(sources, targets, semaphores)
    ]
    for copy in copies:
        copy.start()
    return copies


def finish_loads(copies):
    for copy in copies:
        copy.wait()


def core_now():
    return lax.rem(lax.axis_index("tp"), CORES)


def norm_body(x_ref, gain_ref, ids_ref, route_ref, normed_ref, half_ref, rest_ref):
    value = x_ref[...].astype(jnp.float32)
    scale = lax.rsqrt(jnp.mean(value * value, axis=-1, keepdims=True) + EPSILON)
    normed = (value * scale * gain_ref[...]).astype(jnp.bfloat16)
    normed_ref[...] = normed
    tokens, half = rest_ref.shape
    low, high, first = normed[:, :half], normed[:, half:], core_now() == 0
    half_ref[:tokens, :] = jnp.where(first, low, high)
    rest_ref[...] = jnp.where(first, high, low)
    ids, route = ids_ref[...], route_ref[...]
    extra = half_ref.shape[0] - tokens
    experts = lax.axis_size("ep")
    per_row = half // tokens
    rows = lax.broadcasted_iota(jnp.int32, (extra, half), 0)
    slab = jnp.zeros((extra, half), jnp.float32)
    for row in range(-(-experts // per_row)):
        dense = [
            jnp.sum(jnp.where(ids == row * per_row + e, route, 0.0), axis=0, keepdims=True)
            for e in range(per_row)
        ]
        dense = jnp.concatenate(dense, axis=1)
        coarse = dense.astype(jnp.bfloat16).astype(jnp.float32)
        slab = jnp.where(rows == 2 * row, coarse, slab)
        slab = jnp.where(rows == 2 * row + 1, dense - coarse, slab)
    half_ref[tokens:, :] = slab.astype(jnp.bfloat16)


def expert_weight(ref, tokens):
    expert = lax.axis_index("ep")
    per_row = ref.shape[1] // tokens
    lanes = pl.ds(pl.multiple_of(lax.rem(expert, per_row) * tokens, tokens), tokens)
    slab = ref[tokens:, lanes].astype(jnp.float32).T
    row = lax.broadcasted_iota(jnp.int32, slab.shape, 1) // 2
    wanted = row == lax.div(expert, per_row)
    return jnp.sum(jnp.where(wanted, slab, 0.0), axis=1, keepdims=True)


def silu_product(gate, up):
    return (jax.nn.silu(gate) * up).astype(jnp.bfloat16)


def shared_body(count, normed_ref, *refs):
    sources, outs = refs[: count + 2], refs[count + 2 : 2 * count + 3]
    local, semaphores = refs[2 * count + 3 : 2 * count + 5], refs[2 * count + 5 :]
    copies = start_loads(sources, (*local, *outs[:count]), semaphores)
    normed = normed_ref[...]
    finish_loads(copies[:1])
    gate = dot(normed, local[0][...])
    finish_loads(copies[1:2])
    outs[count][...] = silu_product(gate, dot(normed, local[1][...]))
    finish_loads(copies[2:])


def expert_hidden(tokens, own, other, gate_ref, up_ref):
    half = own[0].shape[1]
    core = core_now()
    low = pl.ds(pl.multiple_of(core * half, half), half)
    high = pl.ds(pl.multiple_of((1 - core) * half, half), half)
    mine = jnp.concatenate([ref[:tokens, :] for ref in own], axis=0)
    theirs = jnp.concatenate([ref[:tokens, :] for ref in other], axis=0)
    gate = dot(mine, gate_ref[0, low, :]) + dot(theirs, gate_ref[0, high, :])
    up = dot(mine, up_ref[0, low, :]) + dot(theirs, up_ref[0, high, :])
    return silu_product(gate, up)


def hidden_body(tokens, count, *refs):
    own, other = refs[:count], refs[count : 2 * count]
    gate_ref, up_ref, out_ref = refs[2 * count :]
    out_ref[...] = expert_hidden(tokens, own, other, gate_ref, up_ref)


def first_hidden_body(tokens, count, loads, *refs):
    own, other = refs[:count], refs[count : 2 * count]
    gate_ref, up_ref, shared_ref = refs[2 * count : 2 * count + 3]
    refs = refs[2 * count + 3 :]
    sources, out_ref, targets = refs[:loads], refs[loads], refs[loads + 1 : 2 * loads + 1]
    copies = start_loads(sources, targets, refs[2 * loads + 1 :])
    rows = count * tokens
    out_ref[:rows, :] = expert_hidden(tokens, own, other, gate_ref, up_ref)
    for strip, columns in shared_strips(out_ref, shared_ref.shape, rows):
        out_ref[columns[0], columns[1]] = shared_ref[strip, :]
    finish_loads(copies)


def shared_strips(ref, shape, first):
    width = shape[1]
    count = ref.shape[1] // width
    height = shape[0] // count
    return [
        (
            slice(i * height, (i + 1) * height),
            (slice(first, first + height), slice(i * width, (i + 1) * width)),
        )
        for i in range(count)
    ]


def quarter_slices(y_count, size):
    index = lax.axis_index("tp")
    y, core = lax.div(index, CORES), lax.rem(index, CORES)
    slices = []
    for side in (core, 1 - core):
        for k in range(y_count):
            start = (lax.rem(y + y_count - k, y_count) * CORES + side) * size
            slices.append(pl.ds(pl.multiple_of(start, size), size))
    return slices


def gathered_dot(pieces, weight, y_count):
    width = pieces[0].shape[1]
    total = None
    for piece, rows in zip(pieces, quarter_slices(y_count, width)):
        part = dot(piece, weight[rows, :])
        total = part if total is None else total + part
    return total


def down_body(y_count, x_count, *refs):
    pieces = refs[: CORES * y_count]
    weight_ref, blocks = refs[CORES * y_count], refs[CORES * y_count + 1 :][:x_count]
    outs = refs[CORES * y_count + 1 + x_count :]
    tokens = outs[0].shape[0]
    rows = x_count * tokens
    total = gathered_dot([piece[:rows, :] for piece in pieces], weight_ref.at[0], y_count)
    total = total.astype(jnp.bfloat16).astype(jnp.float32)
    for r, (block, out) in enumerate(zip(blocks, outs)):
        part = total[r * tokens : (r + 1) * tokens] * expert_weight(block, tokens)
        out[...] = part.astype(out.dtype)


def distance(size, x_count):
    z = lax.div(lax.axis_index("ep"), x_count)
    low = lax.rem(z, size)
    return jnp.where(lax.rem(lax.div(z, size), 2) == 1, low, size - 1 - low)


def pick_body(size, x_count, *refs):
    where = distance(size, x_count)
    refs[-1][...] = pick([ref[...] for ref in refs[:-1]], where)


def base_body(y_count, x_count, *refs):
    pieces, weight_ref = refs[: CORES * y_count], refs[CORES * y_count]
    parts, out_ref = refs[CORES * y_count + 1 : -1], refs[-1]
    tokens = out_ref.shape[0]
    shape = (tokens, weight_ref.shape[0] // (CORES * y_count))
    strips = [where for _, where in shared_strips(pieces[0], shape, x_count * tokens)]
    hidden = [jnp.concatenate([piece[at] for at in strips], axis=0) for piece in pieces]
    total = gathered_dot(hidden, weight_ref, y_count)
    for part in parts:
        total = total + part[...].astype(jnp.float32)
    out_ref[...] = total


def merge_body(y_count, *refs):
    keeps, taken_ref = refs[:y_count], refs[y_count]
    total_ref, sends = refs[y_count + 1], refs[y_count + 2 :]
    for k, send in enumerate(sends, 1):
        send[...] = (keeps[k][...] + taken_ref[k].astype(jnp.float32)).astype(jnp.bfloat16)
    total_ref[...] = keeps[0][...] + taken_ref[0].astype(jnp.float32)


def finish_body(*refs):
    total = refs[0][...]
    for ref in refs[1:-1]:
        total = total + ref[...].astype(jnp.float32)
    refs[-1][...] = total.astype(jnp.bfloat16)


def project_body(y_count, *refs):
    pieces = refs[: CORES * y_count]
    gain_ref, wq_ref, wk_ref, wv_ref, qg_ref, kg_ref, q_ref, kv_ref = refs[CORES * y_count :]
    _, width = pieces[0].shape
    index = lax.axis_index("tp")
    y, core = lax.div(index, CORES), lax.rem(index, CORES)
    query = key = value = squares = None
    number = 0
    for side in (core, 1 - core):
        for k in range(y_count):
            quarter = lax.rem(y + y_count - k, y_count) * CORES + side
            at = pl.ds(pl.multiple_of(quarter * width, width), width)
            x = pieces[number][...].astype(jnp.float32)
            scaled = (x * gain_ref[:, at]).astype(jnp.bfloat16)
            parts = [
                dot(scaled, wq_ref[at, :]),
                dot(scaled, wk_ref[at, :]),
                dot(scaled, wv_ref[at, :]),
                jnp.sum(x * x, axis=1, keepdims=True),
            ]
            if number == 0:
                query, key, value, squares = parts
            else:
                query, key, value, squares = (
                    query + parts[0],
                    key + parts[1],
                    value + parts[2],
                    squares + parts[3],
                )
            number += 1
    inv_rms = lax.rsqrt(squares / (number * width) + EPSILON)
    head_of = lax.broadcasted_iota(jnp.int32, query.shape, 1) // HEAD
    query_squares = query * query
    scale = jnp.zeros_like(query)
    for h in range(query.shape[1] // HEAD):
        mean = jnp.sum(jnp.where(head_of == h, query_squares, 0.0), axis=1, keepdims=True) / HEAD
        scale = jnp.where(head_of == h, lax.rsqrt(mean + EPSILON), scale)
    query_gain = jnp.concatenate([qg_ref[...]] * (query.shape[1] // HEAD), axis=1)
    q_ref[...] = (query * scale * query_gain).astype(jnp.bfloat16)
    kv_index = lax.div(index, lax.axis_size("tp") // KV_HEADS)
    keys = pick([key[:, i * HEAD : (i + 1) * HEAD] for i in range(KV_HEADS)], kv_index)
    values = pick([value[:, i * HEAD : (i + 1) * HEAD] for i in range(KV_HEADS)], kv_index)
    mean = jnp.mean(keys * keys, axis=1, keepdims=True)
    keys = (keys * lax.rsqrt(mean + EPSILON) * kg_ref[...]).astype(jnp.bfloat16)
    kv_ref[...] = jnp.concatenate([keys, (values * inv_rms).astype(jnp.bfloat16)], axis=1)


def attend_body(y_count, q_ref, kv_ref, prev_ref, sink_ref, wo_ref, *outs):
    gives, keeps = outs[0], outs[1:]
    rows, columns = q_ref.shape
    heads = columns // HEAD
    first_row = lax.axis_index("ep") * rows
    head_of = lax.broadcasted_iota(jnp.int32, (WINDOW, columns), 1) // HEAD
    query_at = lax.broadcasted_iota(jnp.int32, (WINDOW, 2 * WINDOW), 0)
    key_at = lax.broadcasted_iota(jnp.int32, (WINDOW, 2 * WINDOW), 1)
    relative = query_at + WINDOW - key_at
    band = (relative >= 0) & (relative < WINDOW)
    head_row = lax.broadcasted_iota(jnp.int32, (heads * WINDOW, 1), 0) // WINDOW
    sink = jnp.zeros((heads * WINDOW, 1), jnp.float32)
    for h in range(heads):
        sink = jnp.where(head_row == h, sink_ref[h], sink)
    attended = []
    for block in range(rows // WINDOW):
        at = block * WINDOW
        own = kv_ref[at : at + WINDOW, :]
        prev = prev_ref[...] if block == 0 else kv_ref[at - WINDOW : at, :]
        both = jnp.concatenate([prev, own], axis=0)
        keys = jnp.concatenate([both[:, :HEAD]] * heads, axis=1)
        values = jnp.concatenate([both[:, HEAD:]] * heads, axis=1)
        queries = q_ref[at : at + WINDOW, :]
        allowed = band & (first_row + at - WINDOW + key_at >= 0)
        allowed = jnp.concatenate([allowed] * heads, axis=0)
        nothing = jnp.zeros_like(queries)
        masked = [jnp.where(head_of == h, queries, nothing) for h in range(heads)]
        scores = lax.dot_general(
            jnp.concatenate(masked, axis=0),
            keys,
            (((1,), (1,)), ((), ())),
            preferred_element_type=jnp.float32,
        ) * HEAD ** (-0.5)
        scores = jnp.where(allowed, scores, -jnp.inf)
        peak = jnp.maximum(jnp.max(scores, axis=1, keepdims=True), sink)
        exponent = jnp.exp(scores - peak)
        total = jnp.sum(exponent, axis=1, keepdims=True) + jnp.exp(sink - peak)
        probability = (exponent / total).astype(jnp.bfloat16)
        spread = dot(probability, values)
        mixed = jnp.zeros((WINDOW, columns), jnp.float32)
        for h in range(heads):
            mixed = jnp.where(head_of == h, spread[h * WINDOW : (h + 1) * WINDOW], mixed)
        attended.append(mixed.astype(jnp.bfloat16))
    attended = jnp.concatenate(attended, axis=0)
    index = lax.axis_index("tp")
    y, core = lax.div(index, CORES), lax.rem(index, CORES)
    width = gives.shape[2]
    for k in range(y_count):
        base = lax.rem(y + k, y_count) * CORES
        at = pl.ds(pl.multiple_of((base + 1 - core) * width, width), width)
        gives[k] = dot(attended, wo_ref[:, at]).astype(jnp.bfloat16)
    for k in range(y_count):
        base = lax.rem(y + k, y_count) * CORES
        at = pl.ds(pl.multiple_of((base + core) * width, width), width)
        keeps[k][...] = dot(attended, wo_ref[:, at])


def shards(
    mixer_input,
    mixer_gain,
    w_query,
    w_key,
    w_value,
    query_gain,
    key_gain,
    sink_logit,
    w_output,
    expert_input,
    expert_gain,
    route_ids,
    route_weight,
    expert_gate,
    expert_up,
    expert_down,
    shared_gate,
    shared_up,
    shared_down,
):
    tp_count = lax.axis_size("tp")
    ep_count = lax.axis_size("ep")
    y_count = tp_count // CORES
    x_count = 1 << ((ep_count.bit_length() - 1) // 2)
    z_count = ep_count // x_count
    bf16, f32 = jnp.bfloat16, jnp.float32
    shape = pltpu.VMEM
    final = jax.ShapeDtypeStruct

    def across(value):
        return lax.ppermute(value, "tp", [(t, t ^ 1) for t in range(tp_count)])

    def turn_y(value, step):
        pairs = [
            (y * CORES + c, (y + step) % y_count * CORES + c)
            for y in range(y_count)
            for c in range(CORES)
        ]
        return lax.ppermute(value, "tp", pairs)

    def swap_ep(value, z_step, x_step):
        pairs = [
            (z * x_count + x, (z ^ z_step) * x_count + (x ^ x_step))
            for z in range(z_count)
            for x in range(x_count)
        ]
        return lax.ppermute(value, "ep", pairs)

    def hop_z(value, size, d):
        moves = []
        for middle in range(size, z_count, 2 * size):
            if d == 0:
                moves += [(middle - 1, middle), (middle, middle - 1)]
            else:
                moves += [(middle - d, middle - d - 1), (middle + d - 1, middle + d)]
        pairs = [
            (source * x_count + x, target * x_count + x)
            for source, target in moves
            for x in range(x_count)
        ]
        return lax.ppermute(value, "ep", pairs)

    def gather_tp(value):
        turned = [value] + [turn_y(value, k) for k in range(1, y_count)]
        return turned + [across(v) for v in turned]

    tokens, width = expert_input.shape
    half = width // CORES
    rows = mixer_input.shape[0]
    piece = width // tp_count
    columns = w_query.shape[1]
    hidden_width = expert_gate.shape[2]
    out_width = expert_down.shape[2]

    mixer_pieces = gather_tp(mixer_input)
    weight_rows = 2 * -(-ep_count * tokens // half)
    weight_rows = -(-weight_rows // SUBLANES) * SUBLANES
    normed, own_half, own_rest = kernel_call(
        norm_body,
        [shape((tokens, width), bf16), shape((tokens + weight_rows, half), bf16)]
        + [shape((tokens, half), bf16)],
        [expert_input, expert_gain.reshape(1, width), route_ids.T, route_weight.T],
        8 * tokens * width,
        8,
    )
    z_blocks = [own_half]
    while len(z_blocks) < z_count:
        size, reached = len(z_blocks), []
        for i in range(size):
            hops, value = [], z_blocks[i]
            for d in range(size):
                value = hop_z(value, size, d)
                hops.append(value)
            reached.append(hops)
        for j in range(size):
            found = [reached[(size - 1) ^ d ^ j][d] for d in range(size)]
            if size > 1:
                found[0] = kernel_call(
                    functools.partial(pick_body, size, x_count),
                    shape(own_half.shape, bf16),
                    vmem(found),
                    1000,
                )
            z_blocks.append(found[0])
    blocks = []
    for s in range(z_count):
        blocks.append([z_blocks[s]] + [swap_ep(z_blocks[s], 0, r) for r in range(1, x_count)])
    others = [
        [across(block) if s or r else own_rest for r, block in enumerate(blocks[s])]
        for s in range(z_count)
    ]
    weights = [expert_gate, expert_up, expert_down]
    shared_width = shared_gate.shape[1]
    gate, up, down, shared_hidden = kernel_call(
        functools.partial(shared_body, len(weights)),
        [shape(weight.shape, bf16) for weight in weights] + [shape((tokens, shared_width), bf16)],
        [("vmem", normed)]
        + [("any", weight) for weight in (shared_gate, shared_up, *weights)],
        4 * tokens * width * shared_width,
        scratch=[pltpu.VMEM(shared_gate.shape, bf16)] * 2
        + [pltpu.SemaphoreType.DMA] * (len(weights) + 2),
    )
    late = [w_query, w_key, w_value, w_output, shared_down]
    hidden0, *late = kernel_call(
        functools.partial(first_hidden_body, tokens, x_count, len(late)),
        [shape((x_count * tokens + tokens * shared_width // hidden_width, hidden_width), bf16)]
        + [shape(weight.shape, bf16) for weight in late],
        vmem(blocks[0] + others[0] + [gate, up, shared_hidden])
        + [("any", weight) for weight in late],
        4 * x_count * tokens * width * hidden_width,
        scratch=[pltpu.SemaphoreType.DMA] * len(late),
    )
    w_query, w_key, w_value, w_output, shared_down = late

    queries, keys_values = kernel_call(
        functools.partial(project_body, y_count),
        [shape((rows, columns), bf16), shape((rows, 2 * HEAD), bf16)],
        [mixer_pieces[0]]
        + vmem(mixer_pieces[1:])
        + [mixer_gain.reshape(1, width)]
        + vmem([w_query, w_key, w_value])
        + [
            query_gain.reshape(1, HEAD),
            key_gain.reshape(1, HEAD),
        ],
        2 * rows * width * (columns + 4 * HEAD),
    )
    before = lax.ppermute(
        keys_values[rows - WINDOW :], "ep", [(i, i + 1) for i in range(ep_count - 1)]
    )
    attended = kernel_call(
        functools.partial(attend_body, y_count),
        [shape((y_count, rows, piece), bf16)] + [shape((rows, piece), f32)] * y_count,
        vmem([queries, keys_values, before]) + [("smem", sink_logit), ("vmem", w_output)],
        2 * rows * columns * width,
    )
    taken = across(attended[0])
    merged = kernel_call(
        functools.partial(merge_body, y_count),
        [shape((rows, piece), f32)] + [shape((rows, piece), bf16)] * (y_count - 1),
        vmem([*attended[1:], taken]),
        rows * width,
    )
    received = [turn_y(sent, k) for k, sent in enumerate(merged[1:], 1)]
    mixer_output = kernel_call(
        finish_body, final((rows, piece), bf16), vmem([merged[0], *received]), rows * width
    )

    returned = []
    for s in range(z_count):
        hidden = hidden0
        if s:
            hidden = kernel_call(
                functools.partial(hidden_body, tokens, x_count),
                shape((x_count * tokens, hidden_width), bf16),
                vmem(blocks[s] + others[s] + [gate, up]),
                4 * x_count * tokens * width * hidden_width,
            )
        pieces = gather_tp(hidden)
        if s == 0:
            shared_pieces = pieces
        own, *sent = kernel_call(
            functools.partial(down_body, y_count, x_count),
            [shape((tokens, out_width), f32)] + [shape((tokens, out_width), bf16)] * (x_count - 1),
            vmem(pieces + [down] + blocks[s]),
            2 * x_count * tokens * expert_down.shape[1] * out_width,
        )
        parts = [own] + [swap_ep(part, 0, r) for r, part in enumerate(sent, 1)]
        if s == 0:
            own_parts = parts
            continue
        summed = kernel_call(
            finish_body, shape((tokens, out_width), bf16), vmem(parts), tokens * out_width
        )
        returned.append(swap_ep(summed, s, 0))
    base = kernel_call(
        functools.partial(base_body, y_count, x_count),
        shape((tokens, out_width), f32),
        vmem(shared_pieces + [shared_down] + own_parts),
        2 * tokens * shared_down.shape[0] * out_width,
    )
    expert_output = kernel_call(
        finish_body, final((tokens, out_width), bf16), vmem([base] + returned), tokens * out_width
    )
    return (mixer_output, expert_output)


def solution(mesh):
    in_specs = (
        P("ep", "tp"),
        P(),
        P(None, "tp"),
        P(),
        P(),
        P(),
        P(),
        P("tp"),
        P("tp", None),
        P("ep", None),
        P(),
        P("ep", None),
        P("ep", None),
        P("ep", None, "tp"),
        P("ep", None, "tp"),
        P("ep", None, "tp"),
        P(None, "tp"),
        P(None, "tp"),
        P(None, "tp"),
    )
    out_specs = (P("ep", "tp"), P("ep", "tp"))

    return jax.shard_map(shards, mesh=mesh, in_specs=in_specs, out_specs=out_specs, check_vma=False)
```
